32 devices in a mesh: grp: 2 (over y), fs: 4 (over z), tp: 4 (over x, core).
Axes of the slice: x: 2, y: 2, z: 4, core: 2. Of those that a mesh axis runs over, the one named last changes fastest.
Arguments:
- prompt: bfloat16 [1024, 2048], P(('grp', 'fs', 'tp')), parts along dimension 0, may hold values from -6 to 6
- norm_gain: float32 [2048], P('fs'), may hold values from 0.1 to 1.9
- up_weight: float32 [2048, 8192], P('fs', 'tp'), may hold values from -0.125 to 0.125
- down_weight: float32 [8192, 2048], P('fs', 'tp'), may hold values from -0.0625 to 0.0625
Outputs:
- up_serving: bfloat16 [4096, 8192], P('grp', 'fs'), parts along dimension 0
- down_serving: bfloat16 [8192, 4096], P('fs', 'grp'), parts along dimension 1
- mlp_output: bfloat16 [1024, 2048], P(('grp', 'fs', 'tp')), parts along dimension 0
The draws below stay inside these ranges and needn't reach their ends.
There are 2 independent parts, one for each index of `grp`. The reference program is written for one: setup_inputs(seed, part) draws one part's arguments, and reference() takes and returns one part's arrays. A program takes and returns all parts, laid end to end along the dimension named above; an argument that names none is the same for every part. Nothing has to cross between parts.
All inputs are finite; a program needn't handle non-finite values.
Results may differ from the reference program's by a relative error of at most 0.024.
Values may be sent and summed in bfloat16 or wider, within the bound.
A program may use at most 128 MiB of HBM per device.

```python
import jax
import jax.numpy as jnp
from jax import lax

D = 2048
FF = 8192
TOKENS = 512
UNITS_DEV = 2048
N_FS = 4


def level_of(key, dims, cuts, least, top_value):
    def one(position, blocks):
        heights = jax.random.uniform(jax.random.fold_in(jax.random.fold_in(key, 6), position), (blocks,), jnp.float32, least / len(cuts), top_value / len(cuts))
        return jnp.repeat(jnp.exp(heights), dims[position] // blocks).reshape((-1,) + (1,) * (len(dims) - position - 1))

    factor_of = one(*cuts[0])
    for cut in cuts[1:]:
        factor_of = factor_of * one(*cut)
    return factor_of


def gaussian(rng, dims, spread, reach, shards=(), kind=jnp.bfloat16):
    array = jax.random.normal(rng, dims, jnp.float32) * spread
    if len(shards) > 0:
        array = level_of(rng, dims, shards, -0.22, 0.18) * array
    return jnp.clip(array, min=-reach, max=reach).astype(kind)


def setup_inputs(seed: int = 0, part: int = 0) -> dict:
    keys = jax.random.split(jax.random.key(seed), 5)
    part_keys = jax.random.split(jax.random.fold_in(keys[4], part), 5)
    return {
        "prompt": gaussian(part_keys[0], (TOKENS, D), 1.0, 6.0, ((0, 16),)),
        "norm_gain": jnp.clip(1.0 + 0.18 * jax.random.normal(keys[1], (D,), jnp.float32), 0.1, 1.9),
        "up_weight": gaussian(keys[2], (D, FF), D ** -0.5, 0.125, ((0, 4), (1, 4)), jnp.float32),
        "down_weight": gaussian(keys[3], (FF, D), FF ** -0.5, 0.0625, ((0, 4), (1, 4)), jnp.float32),
    }


epsilon = 1e-06

def reference(prompt, norm_gain, up_weight, down_weight):
    up_serving = (norm_gain[:, None] * up_weight).astype(jnp.bfloat16)
    down_serving = down_weight.astype(jnp.bfloat16)
    widened = prompt.astype(jnp.float32)
    normed = (widened * lax.rsqrt(lax.optimization_barrier(jnp.mean(widened * widened, axis=-1, keepdims=True)) + epsilon)).astype(jnp.bfloat16)
    projected = jnp.dot(normed, up_serving, preferred_element_type=jnp.float32)
    hidden = jnp.square(jax.nn.relu(projected)).astype(jnp.bfloat16)

    def add_block(summed, block_index):
        offset = (block_index * UNITS_DEV).astype(jnp.int32)
        col_block = lax.dynamic_slice_in_dim(hidden, offset, UNITS_DEV, 1)
        row_block = lax.dynamic_slice_in_dim(down_serving, offset, UNITS_DEV, 0)
        partial_value = jnp.dot(col_block, row_block, preferred_element_type=jnp.float32).astype(jnp.bfloat16)
        partial_value = lax.optimization_barrier(partial_value)
        return (summed + partial_value.astype(jnp.float32), None)
    summed, _ = lax.scan(add_block, jnp.zeros((prompt.shape[0], down_serving.shape[1]), jnp.float32), jnp.arange(N_FS, dtype=jnp.int32))
    return (up_serving, down_serving, summed.astype(jnp.bfloat16))
```

```python
import functools

import jax
import jax.numpy as jnp
from jax import lax
from jax.experimental import pallas as pl
from jax.experimental.pallas import tpu as pltpu
from jax.sharding import PartitionSpec as P

epsilon = 1e-06
CORES = 2
MESH = pl.DeviceIdType.MESH


def kernel(
    groups, fs_count, tp_count, up_steps, down_chunks, down_split,
    ub, db, nb, up_v, down_v, out_v,
    nall, proj, hidden, pbuf, rbuf,
    up_send, up_recv, upf_send, own_send, own_recv,
    dn_send, dn_recv, dnf_send, sib_send, sib_recv,
    n_send, n_recv, r_send, r_recv,
):
    y, z, t = lax.axis_index("grp"), lax.axis_index("fs"), lax.axis_index("tp")
    x, c = t // CORES, lax.rem(t, CORES)
    chips = tp_count // CORES
    ratio, rows, units = ub.shape
    chunk = rows // (up_steps * CORES * groups)
    width = db.shape[1]
    dchunk = units // down_chunks
    tokens = nb.shape[0]
    sibling = (y, z, x * CORES + 1 - c)
    t_src = z // ratio
    x_src, c_src = t_src // CORES, lax.rem(t_src, CORES)
    same_x = x == x_src

    def remote(src, dst, ssem, rsem, dev):
        return pltpu.make_async_remote_copy(
            src_ref=src, dst_ref=dst, send_sem=ssem, recv_sem=rsem, device_id=dev, device_id_type=MESH
        )

    def n_copy(d):
        dst = nall.at[pl.ds(pl.multiple_of(z * tokens, tokens), tokens), :]
        return remote(nb, dst, n_send.at[d], n_recv.at[z], (y, lax.rem(z + d, fs_count), t))

    @pl.loop(1, fs_count)
    def _(d):
        n_copy(d).start()

    def up_at(zr, k):
        return up_v.at[pl.ds(pl.multiple_of(zr * rows + k * chunk, chunk), chunk), :]

    def up_index(m, core, owner):
        return (m * CORES + core) * groups + owner

    def up_first(j, m, cd, dx):
        k = up_index(m, cd, y)
        src = ub.at[j, pl.ds(pl.multiple_of(k * chunk, chunk), chunk), :]
        dev = (y, t * ratio + j, lax.rem(x + dx, chips) * CORES + cd)
        return remote(src, up_at(z, k), up_send.at[j, m, cd, dx], up_recv.at[z, k], dev)

    def up_sends(act):
        for m in range(up_steps):
            for j in range(ratio):
                for cd in range(CORES):
                    for dx in range(1, chips):
                        act(up_first(j, m, cd, dx))

                    @pl.when(t * ratio + j != z)
                    def _():
                        act(up_first(j, m, cd, 0))

    own_j = lax.rem(z, ratio)
    own_rows = pl.ds(pl.multiple_of(z * rows, rows), rows)

    def own_copy():
        return remote(ub.at[own_j], up_v.at[own_rows, :], own_send, own_recv, sibling)

    def sib_copy():
        cols = pl.ds(pl.multiple_of(t * width, width), width)
        return remote(db, down_v.at[:, cols], sib_send, sib_recv, sibling)

    def dn_at(ts, k):
        return down_v.at[
            pl.ds(pl.multiple_of(k * dchunk, dchunk), dchunk), pl.ds(pl.multiple_of(ts * width, width), width)
        ]

    def dn_first(k, dx):
        src = db.at[pl.ds(pl.multiple_of(k * dchunk, dchunk), dchunk), :]
        dev = (y, z, lax.rem(x + dx, chips) * CORES + c)
        return remote(src, dn_at(t, k), dn_send.at[k, dx], dn_recv.at[t, k], dev)

    def dn_sends(act):
        for n in range(down_split):
            for dx in range(1, chips):
                act(dn_first(n * groups + y, dx))
        for k in range(down_split * groups, down_chunks):
            for dx in range(1, chips):
                act(dn_first(k, dx))

    start = lambda copy: copy.start()

    up_sends(start)

    @pl.when(t == t_src)
    def _():
        own_copy().start()

    sib_copy().start()
    dn_sends(start)

    my_cols = pl.ds(pl.multiple_of(t * width, width), width)
    piece = units // down_chunks

    @pl.loop(0, down_chunks)
    def _(i):
        part = pl.ds(pl.multiple_of(i * piece, piece), piece)
        down_v[part, my_cols] = db[part, :]

    @pl.when(t == t_src)
    def _():
        @pl.loop(0, rows // chunk)
        def _(i):
            part = pl.ds(pl.multiple_of(i * chunk, chunk), chunk)
            up_v[pl.ds(pl.multiple_of(z * rows + i * chunk, chunk), chunk), :] = ub[own_j, part, :]

    nall[pl.ds(pl.multiple_of(z * tokens, tokens), tokens), :] = nb[...]

    def up_y(zr, k, g):
        dev = (lax.rem(y + g, groups), z, t)
        return remote(up_at(zr, k), up_at(zr, k), upf_send.at[zr, k, g], up_recv.at[zr, k], dev)

    def up_s(zr, k):
        return remote(up_at(zr, k), up_at(zr, k), upf_send.at[zr, k, 0], up_recv.at[zr, k], sibling)

    def dn_y(ts, k, g):
        dev = (lax.rem(y + g, groups), z, t)
        return remote(dn_at(ts, k), dn_at(ts, k), dnf_send.at[ts, k, g], dn_recv.at[ts, k], dev)

    def dn_s(ts, k):
        return remote(dn_at(ts, k), dn_at(ts, k), dnf_send.at[ts, k, 0], dn_recv.at[ts, k], sibling)

    def if_remote(d, fn):
        if d == 0:
            pl.when(jnp.logical_not(same_x))(fn)
        else:
            fn()

    def up_a(m, d):
        def go():
            zr, k = lax.rem(z + d, fs_count), up_index(m, c, y)
            up_s(zr, k).wait_recv()
            for g in range(1, groups):
                up_y(zr, k, g).start()
            up_s(zr, k).start()

        if_remote(d, go)

    def up_b(m, d):
        def go():
            zr = lax.rem(z + d, fs_count)
            for g in range(1, groups):
                k = up_index(m, c, lax.rem(y + g, groups))
                up_s(zr, k).wait_recv()
                up_s(zr, k).start()

        if_remote(d, go)

    def up_c(d):
        def go():
            zr = lax.rem(z + d, fs_count)
            for m in range(up_steps):
                for owner in range(groups):
                    up_s(zr, up_index(m, 1 - c, owner)).wait_recv()

        if_remote(d, go)

    def up_f(d):
        def go():
            zr = lax.rem(z + d, fs_count)
            for m in range(up_steps):
                for owner in range(groups):
                    up_s(zr, up_index(m, c, owner)).wait_send()
                for g in range(1, groups):
                    up_y(zr, up_index(m, c, y), g).wait_send()

        if_remote(d, go)

    def dn_src(dx):
        return lax.rem(x + dx, chips) * CORES + c

    def dn_a(n, dx):
        ts, k = dn_src(dx), n * groups + y
        dn_s(ts, k).wait_recv()
        for g in range(1, groups):
            dn_y(ts, k, g).start()
        dn_s(ts, k).start()

    def dn_b(n, dx):
        for g in range(1, groups):
            ts, k = dn_src(dx), n * groups + lax.rem(y + g, groups)
            dn_s(ts, k).wait_recv()
            dn_s(ts, k).start()

    def dn_n(k, dx):
        dn_s(dn_src(dx), k).wait_recv()
        dn_s(dn_src(dx), k).start()

    ups = [(m, d) for m in range(up_steps) for d in range(fs_count)]
    lag = fs_count // 2
    for i in range(len(ups) + lag):
        if i < len(ups):
            up_a(*ups[i])
        if i >= lag:
            up_b(*ups[i - lag])
    for n in range(down_split):
        for dx in range(1, chips):
            dn_a(n, dx)

    for d in range(fs_count):
        up_c(d)

    @pl.when(jnp.logical_and(same_x, t != t_src))
    def _():
        own_copy().wait_recv()

    @pl.loop(1, fs_count)
    def _(d):
        zr = lax.rem(z + d, fs_count)
        dst = nall.at[pl.ds(pl.multiple_of(zr * tokens, tokens), tokens), :]
        remote(nb, dst, n_send.at[d], n_recv.at[zr], (y, zr, t)).wait_recv()

    depth = nb.shape[1]
    kb = 256
    nb_tile = min(units, 1024)

    rest = [functools.partial(dn_b, n, dx) for n in range(down_split) for dx in range(1, chips)]
    rest += [
        functools.partial(dn_n, k, dx)
        for k in range(down_split * groups, down_chunks)
        for dx in range(1, chips)
    ]
    pieces = depth // kb
    done = 0
    for i in range(pieces):
        for j in range(units // nb_tile):
            col = pl.ds(j * nb_tile, nb_tile)
            term = jnp.dot(
                nall[:, i * kb : (i + 1) * kb],
                up_v[i * kb : (i + 1) * kb, col],
                preferred_element_type=jnp.float32,
            )
            if i == 0:
                proj[:, col] = term
            else:
                proj[:, col] += term
        upto = len(rest) * (i + 1) // pieces
        for fn in rest[done:upto]:
            fn()
        done = upto

    positive = jnp.maximum(proj[...], 0.0)
    hidden[...] = (positive * positive).astype(jnp.bfloat16)

    def out_copy(ts, d):
        zt = lax.rem(z + d, fs_count)
        cols = pl.ds(pl.multiple_of(ts * width, width), width)
        return remote(pbuf.at[zt, :, cols], rbuf.at[z, :, cols], r_send.at[ts, d], r_recv.at[z, ts], (y, zt, t))

    def block(ts):
        cols = pl.ds(pl.multiple_of(ts * width, width), width)
        part = jnp.dot(hidden[...], down_v[:, cols], preferred_element_type=jnp.float32).astype(jnp.bfloat16)
        pbuf[:, :, cols] = part.reshape(fs_count, tokens, width)

    def send_block(ts):
        @pl.loop(1, fs_count)
        def _(d):
            out_copy(ts, d).start()

    order = [t, x * CORES + 1 - c]
    for dx in range(1, chips):
        order += [dn_src(dx), lax.rem(x + dx, chips) * CORES + 1 - c]
    for i, ts in enumerate(order):
        if i == 1:
            sib_copy().wait_recv()
        if i >= CORES and i % CORES == 1:
            for k in range(down_chunks):
                dn_s(ts, k).wait_recv()
        block(ts)
        if i > 0:
            send_block(order[i - 1])
    send_block(order[-1])

    for d in range(fs_count):
        up_f(d)
    for dx in range(1, chips):
        ts = dn_src(dx)
        for k in range(down_chunks):
            dn_s(ts, k).wait_send()
        for n in range(down_split):
            for g in range(1, groups):
                dn_y(ts, n * groups + y, g).wait_send()
    up_sends(lambda copy: copy.wait_send())
    dn_sends(lambda copy: copy.wait_send())
    sib_copy().wait_send()

    @pl.when(t == t_src)
    def _():
        own_copy().wait_send()

    @pl.loop(1, fs_count)
    def _(d):
        n_copy(d).wait_send()

    total = pbuf[z].astype(jnp.float32)

    @pl.loop(1, fs_count)
    def _(d):
        zr = lax.rem(z + d, fs_count)
        for ts in range(tp_count):
            cols = pl.ds(ts * width, width)
            remote(pbuf.at[zr, :, cols], rbuf.at[zr, :, cols], r_send.at[ts, d], r_recv.at[zr, ts], (y, zr, t)).wait()

    for d in range(1, fs_count):
        total += rbuf[lax.rem(z + d, fs_count)].astype(jnp.float32)
    out_v[...] = total.astype(jnp.bfloat16)


def per_device(groups, prompt, norm_gain, up_weight, down_weight):
    tp_count, fs_count = lax.axis_size("tp"), lax.axis_size("fs")
    rows, wide = up_weight.shape
    units, width = down_weight.shape
    tokens, depth = prompt.shape
    ratio = wide // units
    folded = (norm_gain[:, None] * up_weight).astype(jnp.bfloat16)
    folded = folded.reshape(rows, ratio, units).transpose(1, 0, 2)
    down_local = down_weight.astype(jnp.bfloat16)
    widened = prompt.astype(jnp.float32)
    normed = (
        widened * lax.rsqrt(jnp.mean(widened * widened, axis=-1, keepdims=True) + epsilon)
    ).astype(jnp.bfloat16)
    up_steps = max(1, min(2, rows // (CORES * groups * 16)))
    down_chunks = 8
    down_split = down_chunks // (2 * groups)
    chips = tp_count // CORES
    kc = up_steps * CORES * groups
    dma = pltpu.SemaphoreType.DMA
    vmem = pl.BlockSpec(memory_space=pltpu.VMEM)
    return pl.pallas_call(
        functools.partial(kernel, groups, fs_count, tp_count, up_steps, down_chunks, down_split),
        out_shape=(
            pltpu.VMEM((depth, units), jnp.bfloat16),
            pltpu.VMEM((units, depth), jnp.bfloat16),
            jax.ShapeDtypeStruct((tokens, depth), jnp.bfloat16),
        ),
        in_specs=[vmem] * 3,
        out_specs=(vmem,) * 3,
        scratch_shapes=[
            pltpu.VMEM((fs_count * tokens, depth), jnp.bfloat16),
            pltpu.VMEM((fs_count * tokens, units), jnp.float32),
            pltpu.VMEM((fs_count * tokens, units), jnp.bfloat16),
            pltpu.VMEM((fs_count, tokens, depth), jnp.bfloat16),
            pltpu.VMEM((fs_count, tokens, depth), jnp.bfloat16),
            dma((ratio, up_steps, CORES, chips)),
            dma((fs_count, kc)),
            dma((fs_count, kc, groups)),
            dma, dma,
            dma((down_chunks, chips)),
            dma((tp_count, down_chunks)),
            dma((tp_count, down_chunks, groups)),
            dma, dma,
            dma((fs_count,)),
            dma((fs_count,)),
            dma((tp_count, fs_count)),
            dma((fs_count, tp_count)),
        ],
        compiler_params=pltpu.CompilerParams(has_side_effects=True, vmem_limit_bytes=24 * 1024 * 1024),
    )(folded, down_local, normed)


def solution(mesh):
    return jax.shard_map(
        functools.partial(per_device, mesh.shape["grp"]),
        mesh=mesh,
        in_specs=(P(("grp", "fs", "tp"), None), P("fs"), P("fs", "tp"), P("fs", "tp")),
        out_specs=(P("grp", "fs"), P("fs", "grp"), P(("grp", "fs", "tp"), None)),
        check_vma=False,
    )
```

```python
import functools

import jax
import jax.numpy as jnp
from jax import lax
from jax.experimental import pallas as pl
from jax.experimental.pallas import tpu as pltpu
from jax.sharding import PartitionSpec as P

epsilon = 1e-06
CORES = 2
UP_STEPS = 4
MESH = pl.DeviceIdType.MESH


def kernel(
    groups, fs_count, tp_count, up_steps, down_chunks, down_split,
    ub, db, nb, up_v, down_v, out_v,
    nall, proj, hidden, pbuf, rbuf, stage,
    up_send, stage_recv, z_send, up_recv, upf_send, own_send, own_recv,
    dn_send, dn_recv, dnf_send, sib_send, sib_recv,
    n_send, n_recv, r_send, r_recv,
):
    y, z, t = lax.axis_index("grp"), lax.axis_index("fs"), lax.axis_index("tp")
    x, c = t // CORES, lax.rem(t, CORES)
    chips = tp_count // CORES
    ratio, rows, units = ub.shape
    chunk = rows // (up_steps * CORES * groups)
    width = db.shape[1]
    dchunk = units // down_chunks
    tokens = nb.shape[0]
    sibling = (y, z, x * CORES + 1 - c)
    t_src = z // ratio
    x_src, c_src = t_src // CORES, lax.rem(t_src, CORES)
    same_x = x == x_src

    def remote(src, dst, ssem, rsem, dev):
        return pltpu.make_async_remote_copy(
            src_ref=src, dst_ref=dst, send_sem=ssem, recv_sem=rsem, device_id=dev, device_id_type=MESH
        )

    def n_copy(d):
        dst = nall.at[pl.ds(pl.multiple_of(z * tokens, tokens), tokens), :]
        return remote(nb, dst, n_send.at[d], n_recv.at[z], (y, lax.rem(z + d, fs_count), t))

    @pl.loop(1, fs_count)
    def _(d):
        n_copy(d).start()

    def up_at(zr, k):
        return up_v.at[pl.ds(pl.multiple_of(zr * rows + k * chunk, chunk), chunk), :]

    def up_index(m, core, owner):
        return (m * CORES + core) * groups + owner

    def src_at(j, m, cd):
        k = up_index(m, cd, y)
        return ub.at[j, pl.ds(pl.multiple_of(k * chunk, chunk), chunk), :]

    def up_x(j, m, cd, dx):
        dev = (y, z, lax.rem(x + dx, chips) * CORES + c)
        sem = up_send.at[j, m, cd, dx]
        return remote(src_at(j, m, cd), stage.at[x, j, m, cd], sem, stage_recv.at[x, j, m, cd], dev)

    def up_x_own(j, m, cd, dx):
        dev = (y, z, lax.rem(x + dx, chips) * CORES + cd)
        k = up_index(m, cd, y)
        return remote(src_at(j, m, cd), up_at(z, k), up_send.at[j, m, cd, dx], up_recv.at[z, k], dev)

    def up_x_all(act):
        for m in range(up_steps):
            for cd in range(CORES):
                for j in range(ratio):
                    mine = t * ratio + j == z
                    for dx in range(1, chips):
                        @pl.when(mine)
                        def _():
                            act(up_x_own(j, m, cd, dx))

                        @pl.when(jnp.logical_not(mine))
                        def _():
                            act(up_x(j, m, cd, dx))

    def up_z(j, m, cd, dx):
        xs = lax.rem(x + dx, chips)
        src = src_at(j, m, cd) if dx == 0 else stage.at[xs, j, m, cd]
        k = up_index(m, cd, y)
        dev = (y, (xs * CORES + c) * ratio + j, x * CORES + cd)
        return remote(src, up_at(z, k), z_send.at[j, m, cd, dx], up_recv.at[z, k], dev)

    def up_z_one(j, m, cd, dx, act):
        xs = lax.rem(x + dx, chips)

        @pl.when((xs * CORES + c) * ratio + j != z)
        def _():
            act(j, m, cd, dx)

    def go_z(j, m, cd, dx):
        if dx > 0:
            xs = lax.rem(x + dx, chips)
            at = stage.at[xs, j, m, cd]
            remote(at, at, up_send.at[j, m, cd, dx], stage_recv.at[xs, j, m, cd], sibling).wait_recv()
        up_z(j, m, cd, dx).start()

    own_j = lax.rem(z, ratio)
    own_rows = pl.ds(pl.multiple_of(z * rows, rows), rows)

    def own_copy():
        return remote(ub.at[own_j], up_v.at[own_rows, :], own_send, own_recv, sibling)

    def sib_copy():
        cols = pl.ds(pl.multiple_of(t * width, width), width)
        return remote(db, down_v.at[:, cols], sib_send, sib_recv, sibling)

    def dn_at(ts, k):
        return down_v.at[
            pl.ds(pl.multiple_of(k * dchunk, dchunk), dchunk), pl.ds(pl.multiple_of(ts * width, width), width)
        ]

    def dn_first(k, dx):
        src = db.at[pl.ds(pl.multiple_of(k * dchunk, dchunk), dchunk), :]
        dev = (y, z, lax.rem(x + dx, chips) * CORES + c)
        return remote(src, dn_at(t, k), dn_send.at[k, dx], dn_recv.at[t, k], dev)

    def dn_sends(act):
        for n in range(down_split):
            for dx in range(1, chips):
                act(dn_first(n * groups + y, dx))
        for k in range(down_split * groups, down_chunks):
            for dx in range(1, chips):
                act(dn_first(k, dx))

    start = lambda copy: copy.start()

    for m in range(1):
        for cd in range(CORES):
            for j in range(ratio):
                up_z_one(j, m, cd, 0, go_z)
    up_x_all(start)

    @pl.when(t == t_src)
    def _():
        own_copy().start()

    sib_copy().start()
    dn_sends(start)

    my_cols = pl.ds(pl.multiple_of(t * width, width), width)
    piece = units // down_chunks

    @pl.loop(0, down_chunks)
    def _(i):
        part = pl.ds(pl.multiple_of(i * piece, piece), piece)
        down_v[part, my_cols] = db[part, :]

    @pl.when(t == t_src)
    def _():
        @pl.loop(0, rows // chunk)
        def _(i):
            part = pl.ds(pl.multiple_of(i * chunk, chunk), chunk)
            up_v[pl.ds(pl.multiple_of(z * rows + i * chunk, chunk), chunk), :] = ub[own_j, part, :]

    nall[pl.ds(pl.multiple_of(z * tokens, tokens), tokens), :] = nb[...]

    def up_y(zr, k, g):
        dev = (lax.rem(y + g, groups), z, t)
        return remote(up_at(zr, k), up_at(zr, k), upf_send.at[zr, k, g], up_recv.at[zr, k], dev)

    def up_s(zr, k):
        return remote(up_at(zr, k), up_at(zr, k), upf_send.at[zr, k, 0], up_recv.at[zr, k], sibling)

    def dn_y(ts, k, g):
        dev = (lax.rem(y + g, groups), z, t)
        return remote(dn_at(ts, k), dn_at(ts, k), dnf_send.at[ts, k, g], dn_recv.at[ts, k], dev)

    def dn_s(ts, k):
        return remote(dn_at(ts, k), dn_at(ts, k), dnf_send.at[ts, k, 0], dn_recv.at[ts, k], sibling)

    def if_remote(d, fn):
        if d == 0:
            pl.when(jnp.logical_not(same_x))(fn)
        else:
            fn()

    def up_a(m, d):
        def go():
            zr, k = lax.rem(z + d, fs_count), up_index(m, c, y)
            up_s(zr, k).wait_recv()
            for g in range(1, groups):
                up_y(zr, k, g).start()
            up_s(zr, k).start()

        if_remote(d, go)

    def up_b(m, d):
        def go():
            zr = lax.rem(z + d, fs_count)
            for g in range(1, groups):
                k = up_index(m, c, lax.rem(y + g, groups))
                up_s(zr, k).wait_recv()
                up_s(zr, k).start()

        if_remote(d, go)

    def up_c(d):
        def go():
            zr = lax.rem(z + d, fs_count)
            for m in range(up_steps):
                for owner in range(groups):
                    up_s(zr, up_index(m, 1 - c, owner)).wait_recv()

        if_remote(d, go)

    def up_f(d):
        def go():
            zr = lax.rem(z + d, fs_count)
            for m in range(up_steps):
                for owner in range(groups):
                    up_s(zr, up_index(m, c, owner)).wait_send()
                for g in range(1, groups):
                    up_y(zr, up_index(m, c, y), g).wait_send()

        if_remote(d, go)

    def dn_src(dx):
        return lax.rem(x + dx, chips) * CORES + c

    def dn_a(n, dx):
        ts, k = dn_src(dx), n * groups + y
        dn_s(ts, k).wait_recv()
        for g in range(1, groups):
            dn_y(ts, k, g).start()
        dn_s(ts, k).start()

    def dn_b(n, dx):
        for g in range(1, groups):
            ts, k = dn_src(dx), n * groups + lax.rem(y + g, groups)
            dn_s(ts, k).wait_recv()
            dn_s(ts, k).start()

    def dn_n(k, dx):
        dn_s(dn_src(dx), k).wait_recv()
        dn_s(dn_src(dx), k).start()

    for m in range(up_steps + 2):
        if m < up_steps:
            for cd in range(CORES):
                for j in range(ratio):
                    if m + 1 < up_steps:
                        up_z_one(j, m + 1, cd, 0, go_z)
                    for dx in range(1, chips):
                        up_z_one(j, m, cd, dx, go_z)
        if 1 <= m <= up_steps:
            for d in range(fs_count):
                up_a(m - 1, d)
        if m >= 2:
            for d in range(fs_count):
                up_b(m - 2, d)
    for n in range(down_split):
        for dx in range(1, chips):
            dn_a(n, dx)

    for d in range(fs_count):
        up_c(d)

    @pl.when(jnp.logical_and(same_x, t != t_src))
    def _():
        own_copy().wait_recv()

    @pl.loop(1, fs_count)
    def _(d):
        zr = lax.rem(z + d, fs_count)
        dst = nall.at[pl.ds(pl.multiple_of(zr * tokens, tokens), tokens), :]
        remote(nb, dst, n_send.at[d], n_recv.at[zr], (y, zr, t)).wait_recv()

    depth = nb.shape[1]
    kb = 256
    nb_tile = min(units, 1024)

    rest = [functools.partial(dn_b, n, dx) for n in range(down_split) for dx in range(1, chips)]
    rest += [
        functools.partial(dn_n, k, dx)
        for k in range(down_split * groups, down_chunks)
        for dx in range(1, chips)
    ]
    pieces = depth // kb
    done = 0
    for i in range(pieces):
        for j in range(units // nb_tile):
            col = pl.ds(j * nb_tile, nb_tile)
            term = jnp.dot(
                nall[:, i * kb : (i + 1) * kb],
                up_v[i * kb : (i + 1) * kb, col],
                preferred_element_type=jnp.float32,
            )
            if i == 0:
                proj[:, col] = term
            else:
                proj[:, col] += term
        upto = len(rest) * (i + 1) // pieces
        for fn in rest[done:upto]:
            fn()
        done = upto

    positive = jnp.maximum(proj[...], 0.0)
    hidden[...] = (positive * positive).astype(jnp.bfloat16)

    def out_copy(ts, d):
        zt = lax.rem(z + d, fs_count)
        cols = pl.ds(pl.multiple_of(ts * width, width), width)
        return remote(pbuf.at[zt, :, cols], rbuf.at[z, :, cols], r_send.at[ts, d], r_recv.at[z, ts], (y, zt, t))

    def block(ts):
        cols = pl.ds(pl.multiple_of(ts * width, width), width)
        part = jnp.dot(hidden[...], down_v[:, cols], preferred_element_type=jnp.float32).astype(jnp.bfloat16)
        pbuf[:, :, cols] = part.reshape(fs_count, tokens, width)

    def send_block(ts):
        @pl.loop(1, fs_count)
        def _(d):
            out_copy(ts, d).start()

    order = [t, x * CORES + 1 - c]
    for dx in range(1, chips):
        order += [dn_src(dx), lax.rem(x + dx, chips) * CORES + 1 - c]
    for i, ts in enumerate(order):
        if i == 1:
            sib_copy().wait_recv()
        if i >= CORES and i % CORES == 1:
            for k in range(down_chunks):
                dn_s(ts, k).wait_recv()
        block(ts)
        if i > 0:
            send_block(order[i - 1])
    send_block(order[-1])

    for d in range(fs_count):
        up_f(d)
    for dx in range(1, chips):
        ts = dn_src(dx)
        for k in range(down_chunks):
            dn_s(ts, k).wait_send()
        for n in range(down_split):
            for g in range(1, groups):
                dn_y(ts, n * groups + y, g).wait_send()
    up_x_all(lambda copy: copy.wait_send())
    for m in range(up_steps):
        for cd in range(CORES):
            for j in range(ratio):
                for dx in range(chips):
                    up_z_one(j, m, cd, dx, lambda *at: up_z(*at).wait_send())
    dn_sends(lambda copy: copy.wait_send())
    sib_copy().wait_send()

    @pl.when(t == t_src)
    def _():
        own_copy().wait_send()

    @pl.loop(1, fs_count)
    def _(d):
        n_copy(d).wait_send()

    total = pbuf[z].astype(jnp.float32)

    @pl.loop(1, fs_count)
    def _(d):
        zr = lax.rem(z + d, fs_count)
        for ts in range(tp_count):
            cols = pl.ds(ts * width, width)
            remote(pbuf.at[zr, :, cols], rbuf.at[zr, :, cols], r_send.at[ts, d], r_recv.at[zr, ts], (y, zr, t)).wait()

    for d in range(1, fs_count):
        total += rbuf[lax.rem(z + d, fs_count)].astype(jnp.float32)
    out_v[...] = total.astype(jnp.bfloat16)


def per_device(groups, prompt, norm_gain, up_weight, down_weight):
    tp_count, fs_count = lax.axis_size("tp"), lax.axis_size("fs")
    rows, wide = up_weight.shape
    units, width = down_weight.shape
    tokens, depth = prompt.shape
    ratio = wide // units
    folded = (norm_gain[:, None] * up_weight).astype(jnp.bfloat16)
    folded = folded.reshape(rows, ratio, units).transpose(1, 0, 2)
    down_local = down_weight.astype(jnp.bfloat16)
    widened = prompt.astype(jnp.float32)
    normed = (
        widened * lax.rsqrt(jnp.mean(widened * widened, axis=-1, keepdims=True) + epsilon)
    ).astype(jnp.bfloat16)
    up_steps = max(1, min(UP_STEPS, rows // (CORES * groups * 16)))
    down_chunks = 8
    down_split = down_chunks // (2 * groups)
    chips = tp_count // CORES
    kc = up_steps * CORES * groups
    dma = pltpu.SemaphoreType.DMA
    vmem = pl.BlockSpec(memory_space=pltpu.VMEM)
    return pl.pallas_call(
        functools.partial(kernel, groups, fs_count, tp_count, up_steps, down_chunks, down_split),
        out_shape=(
            pltpu.VMEM((depth, units), jnp.bfloat16),
            pltpu.VMEM((units, depth), jnp.bfloat16),
            jax.ShapeDtypeStruct((tokens, depth), jnp.bfloat16),
        ),
        in_specs=[vmem] * 3,
        out_specs=(vmem,) * 3,
        scratch_shapes=[
            pltpu.VMEM((fs_count * tokens, depth), jnp.bfloat16),
            pltpu.VMEM((fs_count * tokens, units), jnp.float32),
            pltpu.VMEM((fs_count * tokens, units), jnp.bfloat16),
            pltpu.VMEM((fs_count, tokens, depth), jnp.bfloat16),
            pltpu.VMEM((fs_count, tokens, depth), jnp.bfloat16),
            pltpu.VMEM((chips, ratio, up_steps, CORES, rows // kc, units), jnp.bfloat16),
            dma((ratio, up_steps, CORES, chips)),
            dma((chips, ratio, up_steps, CORES)),
            dma((ratio, up_steps, CORES, chips)),
            dma((fs_count, kc)),
            dma((fs_count, kc, groups)),
            dma, dma,
            dma((down_chunks, chips)),
            dma((tp_count, down_chunks)),
            dma((tp_count, down_chunks, groups)),
            dma, dma,
            dma((fs_count,)),
            dma((fs_count,)),
            dma((tp_count, fs_count)),
            dma((fs_count, tp_count)),
        ],
        compiler_params=pltpu.CompilerParams(has_side_effects=True, vmem_limit_bytes=24 * 1024 * 1024),
    )(folded, down_local, normed)


def solution(mesh):
    return jax.shard_map(
        functools.partial(per_device, mesh.shape["grp"]),
        mesh=mesh,
        in_specs=(P(("grp", "fs", "tp"), None), P("fs"), P("fs", "tp"), P("fs", "tp")),
        out_specs=(P("grp", "fs"), P("fs", "grp"), P(("grp", "fs", "tp"), None)),
        check_vma=False,
    )
```

```python
import functools

import jax
import jax.numpy as jnp
from jax import lax
from jax.experimental import pallas as pl
from jax.experimental.pallas import tpu as pltpu
from jax.sharding import PartitionSpec as P

epsilon = 1e-06
CORES = 2
UP_STEPS = 4
DOWN_SPLIT = 0
LAG_A = 1
LAG_B = 3
MESH = pl.DeviceIdType.MESH


def kernel(
    groups, fs_count, tp_count, up_steps, down_chunks, down_split,
    ub, db, nb, up_v, down_v, out_v,
    nall, proj, hidden, pbuf, rbuf, stage,
    up_send, stage_recv, z_send, up_recv, upf_send, own_send, own_recv,
    dn_send, dn_recv, dnf_send, sib_send, sib_recv,
    n_send, n_recv, r_send, r_recv,
):
    y, z, t = lax.axis_index("grp"), lax.axis_index("fs"), lax.axis_index("tp")
    x, c = t // CORES, lax.rem(t, CORES)
    chips = tp_count // CORES
    ratio, rows, units = ub.shape
    chunk = rows // (up_steps * CORES * groups)
    width = db.shape[1]
    dchunk = units // down_chunks
    tokens = nb.shape[0]
    sibling = (y, z, x * CORES + 1 - c)
    t_src = z // ratio
    x_src, c_src = t_src // CORES, lax.rem(t_src, CORES)
    same_x = x == x_src

    def remote(src, dst, ssem, rsem, dev):
        return pltpu.make_async_remote_copy(
            src_ref=src, dst_ref=dst, send_sem=ssem, recv_sem=rsem, device_id=dev, device_id_type=MESH
        )

    def n_copy(d):
        dst = nall.at[pl.ds(pl.multiple_of(z * tokens, tokens), tokens), :]
        return remote(nb, dst, n_send.at[d], n_recv.at[z], (y, lax.rem(z + d, fs_count), t))

    @pl.loop(1, fs_count)
    def _(d):
        n_copy(d).start()

    def up_at(zr, k):
        return up_v.at[pl.ds(pl.multiple_of(zr * rows + k * chunk, chunk), chunk), :]

    def up_index(m, core, owner):
        return (m * CORES + core) * groups + owner

    def src_at(j, m, cd):
        k = up_index(m, cd, y)
        return ub.at[j, pl.ds(pl.multiple_of(k * chunk, chunk), chunk), :]

    def up_x(j, m, cd, dx):
        dev = (y, z, lax.rem(x + dx, chips) * CORES + c)
        sem = up_send.at[j, m, cd, dx]
        return remote(src_at(j, m, cd), stage.at[x, j, m, cd], sem, stage_recv.at[x, j, m, cd], dev)

    def up_x_own(j, m, cd, dx):
        dev = (y, z, lax.rem(x + dx, chips) * CORES + cd)
        k = up_index(m, cd, y)
        return remote(src_at(j, m, cd), up_at(z, k), up_send.at[j, m, cd, dx], up_recv.at[z, k], dev)

    def up_x_all(act):
        for m in range(up_steps):
            for cd in range(CORES):
                for j in range(ratio):
                    mine = t * ratio + j == z
                    for dx in range(1, chips):
                        @pl.when(mine)
                        def _():
                            act(up_x_own(j, m, cd, dx))

                        @pl.when(jnp.logical_not(mine))
                        def _():
                            act(up_x(j, m, cd, dx))

    def up_z(j, m, cd, dx):
        xs = lax.rem(x + dx, chips)
        src = src_at(j, m, cd) if dx == 0 else stage.at[xs, j, m, cd]
        k = up_index(m, cd, y)
        dev = (y, (xs * CORES + c) * ratio + j, x * CORES + cd)
        return remote(src, up_at(z, k), z_send.at[j, m, cd, dx], up_recv.at[z, k], dev)

    def up_z_one(j, m, cd, dx, act):
        xs = lax.rem(x + dx, chips)

        @pl.when((xs * CORES + c) * ratio + j != z)
        def _():
            act(j, m, cd, dx)

    def go_z(j, m, cd, dx):
        if dx > 0:
            xs = lax.rem(x + dx, chips)
            at = stage.at[xs, j, m, cd]
            remote(at, at, up_send.at[j, m, cd, dx], stage_recv.at[xs, j, m, cd], sibling).wait_recv()
        up_z(j, m, cd, dx).start()

    own_j = lax.rem(z, ratio)
    own_rows = pl.ds(pl.multiple_of(z * rows, rows), rows)

    def own_copy():
        return remote(ub.at[own_j], up_v.at[own_rows, :], own_send, own_recv, sibling)

    def sib_copy():
        cols = pl.ds(pl.multiple_of(t * width, width), width)
        return remote(db, down_v.at[:, cols], sib_send, sib_recv, sibling)

    def dn_at(ts, k):
        return down_v.at[
            pl.ds(pl.multiple_of(k * dchunk, dchunk), dchunk), pl.ds(pl.multiple_of(ts * width, width), width)
        ]

    def dn_first(k, dx):
        src = db.at[pl.ds(pl.multiple_of(k * dchunk, dchunk), dchunk), :]
        dev = (y, z, lax.rem(x + dx, chips) * CORES + c)
        return remote(src, dn_at(t, k), dn_send.at[k, dx], dn_recv.at[t, k], dev)

    def dn_sends(act):
        for n in range(down_split):
            for dx in range(1, chips):
                act(dn_first(n * groups + y, dx))
        for k in range(down_split * groups, down_chunks):
            for dx in range(1, chips):
                act(dn_first(k, dx))

    start = lambda copy: copy.start()

    for m in range(1):
        for cd in range(CORES):
            for j in range(ratio):
                up_z_one(j, m, cd, 0, go_z)
    up_x_all(start)

    @pl.when(t == t_src)
    def _():
        own_copy().start()

    sib_copy().start()
    dn_sends(start)

    def up_y(zr, k, g):
        dev = (lax.rem(y + g, groups), z, t)
        return remote(up_at(zr, k), up_at(zr, k), upf_send.at[zr, k, g], up_recv.at[zr, k], dev)

    def up_s(zr, k):
        return remote(up_at(zr, k), up_at(zr, k), upf_send.at[zr, k, 0], up_recv.at[zr, k], sibling)

    def dn_y(ts, k, g):
        dev = (lax.rem(y + g, groups), z, t)
        return remote(dn_at(ts, k), dn_at(ts, k), dnf_send.at[ts, k, g], dn_recv.at[ts, k], dev)

    def dn_s(ts, k):
        return remote(dn_at(ts, k), dn_at(ts, k), dnf_send.at[ts, k, 0], dn_recv.at[ts, k], sibling)

    def if_remote(d, fn):
        if d == 0:
            pl.when(jnp.logical_not(same_x))(fn)
        else:
            fn()

    def up_a(m, d):
        def go():
            zr, k = lax.rem(z + d, fs_count), up_index(m, c, y)
            up_s(zr, k).wait_recv()
            for g in range(1, groups):
                up_y(zr, k, g).start()
            up_s(zr, k).start()

        if_remote(d, go)

    def up_b(m, d):
        def go():
            zr = lax.rem(z + d, fs_count)
            for g in range(1, groups):
                k = up_index(m, c, lax.rem(y + g, groups))
                up_s(zr, k).wait_recv()
                up_s(zr, k).start()

        if_remote(d, go)

    def up_c(d):
        def go():
            zr = lax.rem(z + d, fs_count)
            for m in range(up_steps):
                for owner in range(groups):
                    up_s(zr, up_index(m, 1 - c, owner)).wait_recv()

        if_remote(d, go)

    def up_f(d):
        def go():
            zr = lax.rem(z + d, fs_count)
            for m in range(up_steps):
                for owner in range(groups):
                    up_s(zr, up_index(m, c, owner)).wait_send()
                for g in range(1, groups):
                    up_y(zr, up_index(m, c, y), g).wait_send()

        if_remote(d, go)

    def dn_src(dx):
        return lax.rem(x + dx, chips) * CORES + c

    def dn_a(n, dx):
        ts, k = dn_src(dx), n * groups + y
        dn_s(ts, k).wait_recv()
        for g in range(1, groups):
            dn_y(ts, k, g).start()
        dn_s(ts, k).start()

    def dn_b(n, dx):
        for g in range(1, groups):
            ts, k = dn_src(dx), n * groups + lax.rem(y + g, groups)
            dn_s(ts, k).wait_recv()
            dn_s(ts, k).start()

    def dn_n(k, dx):
        dn_s(dn_src(dx), k).wait_recv()
        dn_s(dn_src(dx), k).start()

    for m in range(up_steps + LAG_B):
        if m < up_steps:
            for cd in range(CORES):
                for j in range(ratio):
                    if m + 1 < up_steps:
                        up_z_one(j, m + 1, cd, 0, go_z)
                    for dx in range(1, chips):
                        up_z_one(j, m, cd, dx, go_z)
        if LAG_A <= m < up_steps + LAG_A:
            for d in range(fs_count):
                up_a(m - LAG_A, d)
        if m >= LAG_B:
            for d in range(fs_count):
                up_b(m - LAG_B, d)
    for n in range(down_split):
        for dx in range(1, chips):
            dn_a(n, dx)

    my_cols = pl.ds(pl.multiple_of(t * width, width), width)
    piece = units // down_chunks

    @pl.loop(0, down_chunks)
    def _(i):
        part = pl.ds(pl.multiple_of(i * piece, piece), piece)
        down_v[part, my_cols] = db[part, :]

    @pl.when(t == t_src)
    def _():
        @pl.loop(0, rows // chunk)
        def _(i):
            part = pl.ds(pl.multiple_of(i * chunk, chunk), chunk)
            up_v[pl.ds(pl.multiple_of(z * rows + i * chunk, chunk), chunk), :] = ub[own_j, part, :]

    nall[pl.ds(pl.multiple_of(z * tokens, tokens), tokens), :] = nb[...]

    for d in range(fs_count):
        up_c(d)

    @pl.when(jnp.logical_and(same_x, t != t_src))
    def _():
        own_copy().wait_recv()

    @pl.loop(1, fs_count)
    def _(d):
        zr = lax.rem(z + d, fs_count)
        dst = nall.at[pl.ds(pl.multiple_of(zr * tokens, tokens), tokens), :]
        remote(nb, dst, n_send.at[d], n_recv.at[zr], (y, zr, t)).wait_recv()

    depth = nb.shape[1]
    kb = 256
    nb_tile = min(units, 1024)

    rest = [functools.partial(dn_b, n, dx) for n in range(down_split) for dx in range(1, chips)]
    rest += [
        functools.partial(dn_n, k, dx)
        for k in range(down_split * groups, down_chunks)
        for dx in range(1, chips)
    ]
    pieces = depth // kb
    done = 0
    for i in range(pieces):
        for j in range(units // nb_tile):
            col = pl.ds(j * nb_tile, nb_tile)
            term = jnp.dot(
                nall[:, i * kb : (i + 1) * kb],
                up_v[i * kb : (i + 1) * kb, col],
                preferred_element_type=jnp.float32,
            )
            if i == 0:
                proj[:, col] = term
            else:
                proj[:, col] += term
        upto = len(rest) * (i + 1) // pieces
        for fn in rest[done:upto]:
            fn()
        done = upto

    positive = jnp.maximum(proj[...], 0.0)
    hidden[...] = (positive * positive).astype(jnp.bfloat16)

    def out_copy(ts, d):
        zt = lax.rem(z + d, fs_count)
        cols = pl.ds(pl.multiple_of(ts * width, width), width)
        return remote(pbuf.at[zt, :, cols], rbuf.at[z, :, cols], r_send.at[ts, d], r_recv.at[z, ts], (y, zt, t))

    def block(ts):
        cols = pl.ds(pl.multiple_of(ts * width, width), width)
        part = jnp.dot(hidden[...], down_v[:, cols], preferred_element_type=jnp.float32).astype(jnp.bfloat16)
        pbuf[:, :, cols] = part.reshape(fs_count, tokens, width)

    def send_block(ts):
        @pl.loop(1, fs_count)
        def _(d):
            out_copy(ts, d).start()

    order = [t, x * CORES + 1 - c]
    for dx in range(1, chips):
        order += [dn_src(dx), lax.rem(x + dx, chips) * CORES + 1 - c]
    for i, ts in enumerate(order):
        if i == 1:
            sib_copy().wait_recv()
        if i >= CORES and i % CORES == 1:
            for k in range(down_chunks):
                dn_s(ts, k).wait_recv()
        block(ts)
        if i > 0:
            send_block(order[i - 1])
    send_block(order[-1])

    for d in range(fs_count):
        up_f(d)
    for dx in range(1, chips):
        ts = dn_src(dx)
        for k in range(down_chunks):
            dn_s(ts, k).wait_send()
        for n in range(down_split):
            for g in range(1, groups):
                dn_y(ts, n * groups + y, g).wait_send()
    up_x_all(lambda copy: copy.wait_send())
    for m in range(up_steps):
        for cd in range(CORES):
            for j in range(ratio):
                for dx in range(chips):
                    up_z_one(j, m, cd, dx, lambda *at: up_z(*at).wait_send())
    dn_sends(lambda copy: copy.wait_send())
    sib_copy().wait_send()

    @pl.when(t == t_src)
    def _():
        own_copy().wait_send()

    @pl.loop(1, fs_count)
    def _(d):
        n_copy(d).wait_send()

    total = pbuf[z].astype(jnp.float32)

    @pl.loop(1, fs_count)
    def _(d):
        zr = lax.rem(z + d, fs_count)
        for ts in range(tp_count):
            cols = pl.ds(ts * width, width)
            remote(pbuf.at[zr, :, cols], rbuf.at[zr, :, cols], r_send.at[ts, d], r_recv.at[zr, ts], (y, zr, t)).wait()

    for d in range(1, fs_count):
        total += rbuf[lax.rem(z + d, fs_count)].astype(jnp.float32)
    out_v[...] = total.astype(jnp.bfloat16)


def per_device(groups, prompt, norm_gain, up_weight, down_weight):
    tp_count, fs_count = lax.axis_size("tp"), lax.axis_size("fs")
    rows, wide = up_weight.shape
    units, width = down_weight.shape
    tokens, depth = prompt.shape
    ratio = wide // units
    folded = (norm_gain[:, None] * up_weight).astype(jnp.bfloat16)
    folded = folded.reshape(rows, ratio, units).transpose(1, 0, 2)
    down_local = down_weight.astype(jnp.bfloat16)
    widened = prompt.astype(jnp.float32)
    normed = (
        widened * lax.rsqrt(jnp.mean(widened * widened, axis=-1, keepdims=True) + epsilon)
    ).astype(jnp.bfloat16)
    up_steps = max(1, min(UP_STEPS, rows // (CORES * groups * 16)))
    down_chunks = 8
    down_split = DOWN_SPLIT
    chips = tp_count // CORES
    kc = up_steps * CORES * groups
    dma = pltpu.SemaphoreType.DMA
    vmem = pl.BlockSpec(memory_space=pltpu.VMEM)
    return pl.pallas_call(
        functools.partial(kernel, groups, fs_count, tp_count, up_steps, down_chunks, down_split),
        out_shape=(
            pltpu.VMEM((depth, units), jnp.bfloat16),
            pltpu.VMEM((units, depth), jnp.bfloat16),
            jax.ShapeDtypeStruct((tokens, depth), jnp.bfloat16),
        ),
        in_specs=[vmem] * 3,
        out_specs=(vmem,) * 3,
        scratch_shapes=[
            pltpu.VMEM((fs_count * tokens, depth), jnp.bfloat16),
            pltpu.VMEM((fs_count * tokens, units), jnp.float32),
            pltpu.VMEM((fs_count * tokens, units), jnp.bfloat16),
            pltpu.VMEM((fs_count, tokens, depth), jnp.bfloat16),
            pltpu.VMEM((fs_count, tokens, depth), jnp.bfloat16),
            pltpu.VMEM((chips, ratio, up_steps, CORES, rows // kc, units), jnp.bfloat16),
            dma((ratio, up_steps, CORES, chips)),
            dma((chips, ratio, up_steps, CORES)),
            dma((ratio, up_steps, CORES, chips)),
            dma((fs_count, kc)),
            dma((fs_count, kc, groups)),
            dma, dma,
            dma((down_chunks, chips)),
            dma((tp_count, down_chunks)),
            dma((tp_count, down_chunks, groups)),
            dma, dma,
            dma((fs_count,)),
            dma((fs_count,)),
            dma((tp_count, fs_count)),
            dma((fs_count, tp_count)),
        ],
        compiler_params=pltpu.CompilerParams(has_side_effects=True, vmem_limit_bytes=24 * 1024 * 1024),
    )(folded, down_local, normed)


def solution(mesh):
    return jax.shard_map(
        functools.partial(per_device, mesh.shape["grp"]),
        mesh=mesh,
        in_specs=(P(("grp", "fs", "tp"), None), P("fs"), P("fs", "tp"), P("fs", "tp")),
        out_specs=(P("grp", "fs"), P("fs", "grp"), P(("grp", "fs", "tp"), None)),
        check_vma=False,
    )
```

```python
import functools

import jax
import jax.numpy as jnp
from jax import lax
from jax.experimental import pallas as pl
from jax.experimental.pallas import tpu as pltpu
from jax.sharding import PartitionSpec as P

epsilon = 1e-06
CORES = 2
PIECES = 4
UP_STEPS = 4
DOWN_SPLIT = 0
LAG_A = 1
LAG_B = 3
MESH = pl.DeviceIdType.MESH


def kernel(
    groups, fs_count, tp_count, up_steps, down_chunks, down_split,
    ub, db, prompt, up_v, down_v, out_v,
    nb, nall, proj, hidden, pbuf, rbuf, stage,
    up_send, stage_recv, z_send, up_recv, upf_send, own_send, own_recv,
    dn_send, dn_recv, dnf_send, sib_send, sib_recv,
    n_send, n_recv, r_send, r_recv,
):
    y, z, t = lax.axis_index("grp"), lax.axis_index("fs"), lax.axis_index("tp")
    x, c = t // CORES, lax.rem(t, CORES)
    chips = tp_count // CORES
    ratio, rows, units = ub.shape
    chunk = rows // (up_steps * CORES * groups)
    width = db.shape[1]
    dchunk = units // down_chunks
    tokens = prompt.shape[0]
    sibling = (y, z, x * CORES + 1 - c)
    t_src = z // ratio
    x_src, c_src = t_src // CORES, lax.rem(t_src, CORES)
    same_x = x == x_src

    def remote(src, dst, ssem, rsem, dev):
        return pltpu.make_async_remote_copy(
            src_ref=src, dst_ref=dst, send_sem=ssem, recv_sem=rsem, device_id=dev, device_id_type=MESH
        )

    def n_copy(d):
        dst = nall.at[pl.ds(pl.multiple_of(z * tokens, tokens), tokens), :]
        return remote(nb, dst, n_send.at[d], n_recv.at[z], (y, lax.rem(z + d, fs_count), t))

    def up_at(zr, k):
        return up_v.at[pl.ds(pl.multiple_of(zr * rows + k * chunk, chunk), chunk), :]

    def up_index(m, core, owner):
        return (m * CORES + core) * groups + owner

    def src_at(j, m, cd):
        k = up_index(m, cd, y)
        return ub.at[j, pl.ds(pl.multiple_of(k * chunk, chunk), chunk), :]

    def up_x(j, m, cd, dx):
        dev = (y, z, lax.rem(x + dx, chips) * CORES + c)
        sem = up_send.at[j, m, cd, dx]
        return remote(src_at(j, m, cd), stage.at[x, j, m, cd], sem, stage_recv.at[x, j, m, cd], dev)

    def up_x_own(j, m, cd, dx):
        dev = (y, z, lax.rem(x + dx, chips) * CORES + cd)
        k = up_index(m, cd, y)
        return remote(src_at(j, m, cd), up_at(z, k), up_send.at[j, m, cd, dx], up_recv.at[z, k], dev)

    def up_x_all(act):
        for m in range(up_steps):
            for cd in range(CORES):
                for j in range(ratio):
                    mine = t * ratio + j == z
                    for dx in range(1, chips):
                        @pl.when(mine)
                        def _():
                            act(up_x_own(j, m, cd, dx))

                        @pl.when(jnp.logical_not(mine))
                        def _():
                            act(up_x(j, m, cd, dx))

    def up_z(j, m, cd, dx):
        xs = lax.rem(x + dx, chips)
        src = src_at(j, m, cd) if dx == 0 else stage.at[xs, j, m, cd]
        k = up_index(m, cd, y)
        dev = (y, (xs * CORES + c) * ratio + j, x * CORES + cd)
        return remote(src, up_at(z, k), z_send.at[j, m, cd, dx], up_recv.at[z, k], dev)

    def up_z_one(j, m, cd, dx, act):
        xs = lax.rem(x + dx, chips)

        @pl.when((xs * CORES + c) * ratio + j != z)
        def _():
            act(j, m, cd, dx)

    def go_z(j, m, cd, dx):
        if dx > 0:
            xs = lax.rem(x + dx, chips)
            at = stage.at[xs, j, m, cd]
            remote(at, at, up_send.at[j, m, cd, dx], stage_recv.at[xs, j, m, cd], sibling).wait_recv()
        up_z(j, m, cd, dx).start()

    own_j = lax.rem(z, ratio)
    own_rows = pl.ds(pl.multiple_of(z * rows, rows), rows)

    def own_copy():
        return remote(ub.at[own_j], up_v.at[own_rows, :], own_send, own_recv, sibling)

    def sib_copy():
        cols = pl.ds(pl.multiple_of(t * width, width), width)
        return remote(db, down_v.at[:, cols], sib_send, sib_recv, sibling)

    def dn_at(ts, k):
        return down_v.at[
            pl.ds(pl.multiple_of(k * dchunk, dchunk), dchunk), pl.ds(pl.multiple_of(ts * width, width), width)
        ]

    def dn_first(k, dx):
        src = db.at[pl.ds(pl.multiple_of(k * dchunk, dchunk), dchunk), :]
        dev = (y, z, lax.rem(x + dx, chips) * CORES + c)
        return remote(src, dn_at(t, k), dn_send.at[k, dx], dn_recv.at[t, k], dev)

    def dn_sends(act):
        for n in range(down_split):
            for dx in range(1, chips):
                act(dn_first(n * groups + y, dx))
        for k in range(down_split * groups, down_chunks):
            for dx in range(1, chips):
                act(dn_first(k, dx))

    start = lambda copy: copy.start()

    for m in range(1):
        for cd in range(CORES):
            for j in range(ratio):
                up_z_one(j, m, cd, 0, go_z)
    up_x_all(start)

    @pl.when(t == t_src)
    def _():
        own_copy().start()

    sib_copy().start()
    dn_sends(start)

    widened = prompt[...].astype(jnp.float32)
    scale = lax.rsqrt(jnp.mean(widened * widened, axis=-1, keepdims=True) + epsilon)
    nb[...] = (widened * scale).astype(jnp.bfloat16)

    def up_y(zr, k, g):
        dev = (lax.rem(y + g, groups), z, t)
        return remote(up_at(zr, k), up_at(zr, k), upf_send.at[zr, k, g], up_recv.at[zr, k], dev)

    def up_s(zr, k):
        return remote(up_at(zr, k), up_at(zr, k), upf_send.at[zr, k, 0], up_recv.at[zr, k], sibling)

    def dn_y(ts, k, g):
        dev = (lax.rem(y + g, groups), z, t)
        return remote(dn_at(ts, k), dn_at(ts, k), dnf_send.at[ts, k, g], dn_recv.at[ts, k], dev)

    def dn_s(ts, k):
        return remote(dn_at(ts, k), dn_at(ts, k), dnf_send.at[ts, k, 0], dn_recv.at[ts, k], sibling)

    def if_remote(d, fn):
        if d == 0:
            pl.when(jnp.logical_not(same_x))(fn)
        else:
            fn()

    def up_a(m, d):
        def go():
            zr, k = lax.rem(z + d, fs_count), up_index(m, c, y)
            up_s(zr, k).wait_recv()
            for g in range(1, groups):
                up_y(zr, k, g).start()
            up_s(zr, k).start()

        if_remote(d, go)

    def up_b(m, d):
        def go():
            zr = lax.rem(z + d, fs_count)
            for g in range(1, groups):
                k = up_index(m, c, lax.rem(y + g, groups))
                up_s(zr, k).wait_recv()
                up_s(zr, k).start()

        if_remote(d, go)

    def up_c(d):
        def go():
            zr = lax.rem(z + d, fs_count)
            for m in range(up_steps):
                for owner in range(groups):
                    up_s(zr, up_index(m, 1 - c, owner)).wait_recv()

        if_remote(d, go)

    def up_f(d):
        def go():
            zr = lax.rem(z + d, fs_count)
            for m in range(up_steps):
                for owner in range(groups):
                    up_s(zr, up_index(m, c, owner)).wait_send()
                for g in range(1, groups):
                    up_y(zr, up_index(m, c, y), g).wait_send()

        if_remote(d, go)

    def dn_src(dx):
        return lax.rem(x + dx, chips) * CORES + c

    def dn_a(n, dx):
        ts, k = dn_src(dx), n * groups + y
        dn_s(ts, k).wait_recv()
        for g in range(1, groups):
            dn_y(ts, k, g).start()
        dn_s(ts, k).start()

    def dn_b(n, dx):
        for g in range(1, groups):
            ts, k = dn_src(dx), n * groups + lax.rem(y + g, groups)
            dn_s(ts, k).wait_recv()
            dn_s(ts, k).start()

    def dn_n(k, dx):
        dn_s(dn_src(dx), k).wait_recv()
        dn_s(dn_src(dx), k).start()

    for m in range(up_steps + LAG_B):
        if m < up_steps:
            for cd in range(CORES):
                for j in range(ratio):
                    if m + 1 < up_steps:
                        up_z_one(j, m + 1, cd, 0, go_z)
                    for dx in range(1, chips):
                        up_z_one(j, m, cd, dx, go_z)
        if LAG_A <= m < up_steps + LAG_A:
            for d in range(fs_count):
                up_a(m - LAG_A, d)
        if m >= LAG_B:
            for d in range(fs_count):
                up_b(m - LAG_B, d)
    for n in range(down_split):
        for dx in range(1, chips):
            dn_a(n, dx)

    my_cols = pl.ds(pl.multiple_of(t * width, width), width)
    piece = units // down_chunks

    @pl.loop(0, down_chunks)
    def _(i):
        part = pl.ds(pl.multiple_of(i * piece, piece), piece)
        down_v[part, my_cols] = db[part, :]

    @pl.when(t == t_src)
    def _():
        @pl.loop(0, rows // chunk)
        def _(i):
            part = pl.ds(pl.multiple_of(i * chunk, chunk), chunk)
            up_v[pl.ds(pl.multiple_of(z * rows + i * chunk, chunk), chunk), :] = ub[own_j, part, :]

    nall[pl.ds(pl.multiple_of(z * tokens, tokens), tokens), :] = nb[...]

    @pl.loop(1, fs_count)
    def _(d):
        n_copy(d).start()

    for d in range(fs_count):
        up_c(d)

    @pl.when(jnp.logical_and(same_x, t != t_src))
    def _():
        own_copy().wait_recv()

    @pl.loop(1, fs_count)
    def _(d):
        zr = lax.rem(z + d, fs_count)
        dst = nall.at[pl.ds(pl.multiple_of(zr * tokens, tokens), tokens), :]
        remote(nb, dst, n_send.at[d], n_recv.at[zr], (y, zr, t)).wait_recv()

    depth = prompt.shape[1]
    kb = 256
    nb_tile = min(units, 1024)

    rest = [functools.partial(dn_b, n, dx) for n in range(down_split) for dx in range(1, chips)]
    rest += [
        functools.partial(dn_n, k, dx)
        for k in range(down_split * groups, down_chunks)
        for dx in range(1, chips)
    ]
    pieces = depth // kb
    done = 0
    for i in range(pieces):
        for j in range(units // nb_tile):
            col = pl.ds(j * nb_tile, nb_tile)
            term = jnp.dot(
                nall[:, i * kb : (i + 1) * kb],
                up_v[i * kb : (i + 1) * kb, col],
                preferred_element_type=jnp.float32,
            )
            if i == 0:
                proj[:, col] = term
            else:
                proj[:, col] += term
        upto = len(rest) * (i + 1) // pieces
        for fn in rest[done:upto]:
            fn()
        done = upto

    positive = jnp.maximum(proj[...], 0.0)
    hidden[...] = (positive * positive).astype(jnp.bfloat16)

    def out_copy(ts, d):
        zt = lax.rem(z + d, fs_count)
        cols = pl.ds(pl.multiple_of(ts * width, width), width)
        return remote(pbuf.at[zt, :, cols], rbuf.at[z, :, cols], r_send.at[ts, d], r_recv.at[z, ts], (y, zt, t))

    def block(ts):
        cols = pl.ds(pl.multiple_of(ts * width, width), width)
        part = jnp.dot(hidden[...], down_v[:, cols], preferred_element_type=jnp.float32).astype(jnp.bfloat16)
        pbuf[:, :, cols] = part.reshape(fs_count, tokens, width)

    def send_block(ts):
        @pl.loop(1, fs_count)
        def _(d):
            out_copy(ts, d).start()

    order = [t, x * CORES + 1 - c]
    for dx in range(1, chips):
        order += [dn_src(dx), lax.rem(x + dx, chips) * CORES + 1 - c]
    for i, ts in enumerate(order):
        if i == 1:
            sib_copy().wait_recv()
        if i >= CORES and i % CORES == 1:
            for k in range(down_chunks):
                dn_s(ts, k).wait_recv()
        block(ts)
        if i > 0:
            send_block(order[i - 1])
    send_block(order[-1])

    for d in range(fs_count):
        up_f(d)
    for dx in range(1, chips):
        ts = dn_src(dx)
        for k in range(down_chunks):
            dn_s(ts, k).wait_send()
        for n in range(down_split):
            for g in range(1, groups):
                dn_y(ts, n * groups + y, g).wait_send()
    up_x_all(lambda copy: copy.wait_send())
    for m in range(up_steps):
        for cd in range(CORES):
            for j in range(ratio):
                for dx in range(chips):
                    up_z_one(j, m, cd, dx, lambda *at: up_z(*at).wait_send())
    dn_sends(lambda copy: copy.wait_send())
    sib_copy().wait_send()

    @pl.when(t == t_src)
    def _():
        own_copy().wait_send()

    @pl.loop(1, fs_count)
    def _(d):
        n_copy(d).wait_send()

    total = pbuf[z].astype(jnp.float32)

    @pl.loop(1, fs_count)
    def _(d):
        zr = lax.rem(z + d, fs_count)
        for ts in range(tp_count):
            cols = pl.ds(ts * width, width)
            remote(pbuf.at[zr, :, cols], rbuf.at[zr, :, cols], r_send.at[ts, d], r_recv.at[zr, ts], (y, zr, t)).wait()

    for d in range(1, fs_count):
        total += rbuf[lax.rem(z + d, fs_count)].astype(jnp.float32)
    out_v[...] = total.astype(jnp.bfloat16)


def write_out(up_v, down_v, out_v, up_out, down_out, mlp_out, sems):
    copies = [pltpu.make_async_copy(out_v, mlp_out, sems.at[2 * PIECES])]
    for n, (src, dst) in enumerate(((up_v, up_out), (down_v, down_out))):
        step = src.shape[0] // PIECES
        for i in range(PIECES):
            part = pl.ds(i * step, step)
            copies.append(pltpu.make_async_copy(src.at[part, :], dst.at[part, :], sems.at[n * PIECES + i]))
    for copy in copies:
        copy.start()
    for copy in copies:
        copy.wait()


def per_device(groups, prompt, norm_gain, up_weight, down_weight):
    tp_count, fs_count = lax.axis_size("tp"), lax.axis_size("fs")
    rows, wide = up_weight.shape
    units, width = down_weight.shape
    tokens, depth = prompt.shape
    ratio = wide // units
    folded = (norm_gain[:, None] * up_weight).astype(jnp.bfloat16)
    folded = folded.reshape(rows, ratio, units).transpose(1, 0, 2)
    down_local = down_weight.astype(jnp.bfloat16)
    up_steps = max(1, min(UP_STEPS, rows // (CORES * groups * 16)))
    down_chunks = 8
    down_split = DOWN_SPLIT
    chips = tp_count // CORES
    kc = up_steps * CORES * groups
    dma = pltpu.SemaphoreType.DMA
    vmem = pl.BlockSpec(memory_space=pltpu.VMEM)
    up_v, down_v, out_v = pl.pallas_call(
        functools.partial(kernel, groups, fs_count, tp_count, up_steps, down_chunks, down_split),
        out_shape=(
            pltpu.VMEM((depth, units), jnp.bfloat16),
            pltpu.VMEM((units, depth), jnp.bfloat16),
            jax.ShapeDtypeStruct((tokens, depth), jnp.bfloat16),
        ),
        in_specs=[vmem] * 3,
        out_specs=(vmem,) * 3,
        scratch_shapes=[
            pltpu.VMEM((tokens, depth), jnp.bfloat16),
            pltpu.VMEM((fs_count * tokens, depth), jnp.bfloat16),
            pltpu.VMEM((fs_count * tokens, units), jnp.float32),
            pltpu.VMEM((fs_count * tokens, units), jnp.bfloat16),
            pltpu.VMEM((fs_count, tokens, depth), jnp.bfloat16),
            pltpu.VMEM((fs_count, tokens, depth), jnp.bfloat16),
            pltpu.VMEM((chips, ratio, up_steps, CORES, rows // kc, units), jnp.bfloat16),
            dma((ratio, up_steps, CORES, chips)),
            dma((chips, ratio, up_steps, CORES)),
            dma((ratio, up_steps, CORES, chips)),
            dma((fs_count, kc)),
            dma((fs_count, kc, groups)),
            dma, dma,
            dma((down_chunks, chips)),
            dma((tp_count, down_chunks)),
            dma((tp_count, down_chunks, groups)),
            dma, dma,
            dma((fs_count,)),
            dma((fs_count,)),
            dma((tp_count, fs_count)),
            dma((fs_count, tp_count)),
        ],
        compiler_params=pltpu.CompilerParams(has_side_effects=True, vmem_limit_bytes=24 * 1024 * 1024),
    )(folded, down_local, prompt)
    any_space = pl.BlockSpec(memory_space=pl.ANY)
    return pl.pallas_call(
        write_out,
        out_shape=(
            jax.ShapeDtypeStruct(up_v.shape, jnp.bfloat16),
            jax.ShapeDtypeStruct(down_v.shape, jnp.bfloat16),
            jax.ShapeDtypeStruct(out_v.shape, jnp.bfloat16),
        ),
        in_specs=[vmem] * 3,
        out_specs=(any_space,) * 3,
        scratch_shapes=[dma((2 * PIECES + 1,))],
        compiler_params=pltpu.CompilerParams(vmem_limit_bytes=1024 * 1024),
        cost_estimate=pl.CostEstimate(flops=0, bytes_accessed=4 * depth * units * 2, transcendentals=0),
    )(up_v, down_v, out_v)


def solution(mesh):
    return jax.shard_map(
        functools.partial(per_device, mesh.shape["grp"]),
        mesh=mesh,
        in_specs=(P(("grp", "fs", "tp"), None), P("fs"), P("fs", "tp"), P("fs", "tp")),
        out_specs=(P("grp", "fs"), P("fs", "grp"), P(("grp", "fs", "tp"), None)),
        check_vma=False,
    )
```
